32 devices in a mesh: sp: 8 (over z, y), tp: 4 (over x, core).
Axes of the slice: x: 2, y: 2, z: 4, core: 2. Of those that a mesh axis runs over, the one named last changes fastest.
Arguments:
- layer_source: bfloat16 [8192, 2048], P(('sp', 'tp')), may hold values from -6 to 6
- broad_probe_tensor: bfloat16 [8192, 512], P('sp', 'tp'), may hold values from -6 to 6
- broad_retention_preact: bfloat16 [8192, 512], P('sp', 'tp'), may hold values from -6 to 6
- broad_floor_margin: float32 [512], P('tp'), may hold values from 3.6621094e-05 to 0.12
- slim_probe_tensor: bfloat16 [8192, 256], P('sp', 'tp'), may hold values from -6 to 6
- slim_retention_preact: bfloat16 [8192, 256], P('sp', 'tp'), may hold values from -6 to 6
- slim_floor_margin: float32 [256], P('tp'), may hold values from 3.6621094e-05 to 0.12
- branch_content_tensor: bfloat16 [2, 8192, 512], P(None, 'sp', 'tp'), may hold values from -6 to 6
- emitted_switch_preact: bfloat16 [2, 8192, 512], P(None, 'sp', 'tp'), may hold values from -6 to 6
- extra_log_fades: float32 [2, 8192, 4], P(None, 'sp', 'tp'), may hold values from -1.4 to 0
- channel_norm_scale: float32 [128], replicated, may hold values from 0.1 to 1.9
- emission_projection: bfloat16 [2, 512, 2048], replicated, may hold values from -0.1875 to 0.1875
- mlp_norm_scale: float32 [2048], replicated, may hold values from 0.1 to 1.9
- switch_projection: bfloat16 [2048, 5632], P('sp', 'tp'), may hold values from -0.125 to 0.125
- expand_projection: bfloat16 [2048, 5632], P('sp', 'tp'), may hold values from -0.125 to 0.125
- shrink_projection: bfloat16 [5632, 2048], P('tp', 'sp'), may hold values from -0.078125 to 0.078125
Outputs:
- layer_out: bfloat16 [8192, 2048], P(('sp', 'tp'))
The draws below stay inside these ranges and needn't reach their ends.
All inputs are finite; a program needn't handle non-finite values.
Results may differ from the reference program's by a relative error of at most 0.0095.
Values may be sent and summed in bfloat16 or wider, within the bound.
A program may use at most 192 MiB of HBM per device.

```python
import jax
import jax.numpy as jnp
from jax import lax

D = 2048
FF = 5632
BRANCH_CHANNELS = 4
KW = 128
KN = 64
DV = 128
BLOCK = 64
TOK_DEV = 1024
TOKENS = 8192


def forget_draw(key, key_width):
    block_rows = TOK_DEV // 2
    block_count = TOKENS // block_rows
    noise = jax.random.normal(key, (TOKENS, BRANCH_CHANNELS * key_width), jnp.float32)
    offsets = jax.random.uniform(jax.random.fold_in(key, 7), (block_count, 1, BRANCH_CHANNELS, 1), jnp.float32, -1.5, 1.5)
    shaped = noise.reshape(block_count, block_rows, BRANCH_CHANNELS, key_width) + offsets
    return jnp.clip(shaped.reshape(TOKENS, BRANCH_CHANNELS * key_width), -6.0, 6.0).astype(jnp.bfloat16)


def gap_draw(key, key_width):
    order = jax.random.permutation(jax.random.fold_in(key, 3), BRANCH_CHANNELS)
    slow_count = BRANCH_CHANNELS // 2
    slow_heads = (order < slow_count)[:, None]
    spread = jax.random.uniform(jax.random.fold_in(key, 5), (BRANCH_CHANNELS, key_width), jnp.float32)
    slow_gap = jnp.exp(jnp.log(0.3 / TOKENS) + spread * jnp.log(5.0))
    fast_gap = jnp.exp(jnp.log(0.04) + spread * jnp.log(3.0))
    return jnp.where(slow_heads, slow_gap, fast_gap).reshape(BRANCH_CHANNELS * key_width)


def draw_broad_retention_preact(key, part):
    return forget_draw(key, KW)


def draw_slim_retention_preact(key, part):
    return forget_draw(key, KN)


def draw_broad_floor_margin(key, part):
    return gap_draw(key, KW)


def draw_slim_floor_margin(key, part):
    return gap_draw(key, KN)


def draw_extra_log_fades(key, part):
    picks = jax.random.randint(key, (2, 2, BRANCH_CHANNELS), 0, TOKENS)
    amounts = jax.random.uniform(jax.random.fold_in(key, 11), (2, 2, BRANCH_CHANNELS), jnp.float32, jnp.log(0.5), jnp.log(0.8))
    matched = jnp.arange(TOKENS)[None, None, :, None] == picks[:, :, None, :]
    return jnp.sum(jnp.where(matched, amounts[:, :, None, :], 0.0), axis=1)


def level_of(own_key, dims, cuts, least, high):
    loudness = 1.0
    for position, shards_of in cuts:
        steps = jax.random.uniform(jax.random.fold_in(jax.random.fold_in(own_key, 6), position), (shards_of,), jnp.float32, least / len(cuts), high / len(cuts))
        loudness = loudness * jnp.repeat(jnp.exp(steps), dims[position] // shards_of).reshape((-1,) + (1,) * (len(dims) - 1 - position))
    return loudness


def gaussian(key, shape, scale, most, pieces=(), kind=jnp.bfloat16):
    values = scale * jax.random.normal(key, shape, jnp.float32)
    if pieces:
        values = values * level_of(key, shape, pieces, -0.22, 0.18)
    return jnp.clip(values, -most, most).astype(kind)


def setup_inputs(seed: int = 0) -> dict:
    seeds = jax.random.split(jax.random.key(seed), 17)
    return {
        "layer_source": gaussian(seeds[0], (TOKENS, D), 1.0, 6.0, ((0, 32),)),
        "broad_probe_tensor": gaussian(seeds[1], (TOKENS, BRANCH_CHANNELS * KW), 1.0, 6.0, ((0, 8), (1, 4))),
        "broad_retention_preact": draw_broad_retention_preact(jax.random.fold_in(seeds[16], 71), 0),
        "broad_floor_margin": draw_broad_floor_margin(jax.random.fold_in(seeds[16], 71), 0),
        "slim_probe_tensor": gaussian(seeds[4], (TOKENS, BRANCH_CHANNELS * KN), 1.0, 6.0, ((0, 8), (1, 4))),
        "slim_retention_preact": draw_slim_retention_preact(jax.random.fold_in(seeds[16], 71), 0),
        "slim_floor_margin": draw_slim_floor_margin(jax.random.fold_in(seeds[16], 71), 0),
        "branch_content_tensor": gaussian(seeds[7], (2, TOKENS, BRANCH_CHANNELS * DV), 1.0, 6.0, ((1, 8), (2, 4))),
        "emitted_switch_preact": gaussian(seeds[8], (2, TOKENS, BRANCH_CHANNELS * DV), 1.0, 6.0, ((1, 8), (2, 4))),
        "extra_log_fades": draw_extra_log_fades(jax.random.fold_in(seeds[16], 71), 0),
        "channel_norm_scale": jnp.clip(1.0 + 0.18 * jax.random.normal(seeds[10], (DV,), jnp.float32), 0.1, 1.9),
        "emission_projection": gaussian(seeds[11], (2, BRANCH_CHANNELS * DV, D), (2 * BRANCH_CHANNELS * DV) ** -0.5, 0.1875),
        "mlp_norm_scale": jnp.clip(1.0 + 0.18 * jax.random.normal(seeds[12], (D,), jnp.float32), 0.1, 1.9),
        "switch_projection": gaussian(seeds[13], (D, FF), D ** -0.5, 0.125, ((0, 8), (1, 4))),
        "expand_projection": gaussian(seeds[14], (D, FF), D ** -0.5, 0.125, ((0, 8), (1, 4))),
        "shrink_projection": gaussian(seeds[15], (FF, D), FF ** -0.5, 0.078125, ((0, 4), (1, 8))),
    }


EPSILON = 1e-06
EXACT_PRECISION = lax.Precision.HIGHEST

def switched_token_entries(probe_array, retention_sigmoid, floor_margin, spike_rows, rows_of_values, count_heads):
    length = probe_array.shape[0]
    key_width = probe_array.shape[1] // count_heads
    shaped = retention_sigmoid.astype(jnp.float32).reshape(length, count_heads, key_width)
    address_entries = floor_margin.reshape(count_heads, key_width) * jax.nn.sigmoid(-shaped)
    log_fade_amount = jnp.log1p(-address_entries) + spike_rows[:, :, None]
    probe_entries = jax.nn.silu(probe_array.astype(jnp.float32)).reshape(length, count_heads, key_width) * key_width ** (-0.5)
    content_arrays = rows_of_values.astype(jnp.float32).reshape(length, count_heads, -1)
    return (probe_entries, address_entries, log_fade_amount, content_arrays)

def block_recurrence(probe_entries, address_entries, log_fade_amount, content_arrays, block_len):
    length, count_heads, key_width = probe_entries.shape
    value_width = content_arrays.shape[2]
    block_count = length // block_len

    def to_blocks(tensor):
        return jnp.moveaxis(tensor.reshape(block_count, block_len, count_heads, tensor.shape[2]), 2, 1)
    causal_mask = jnp.tril(jnp.ones((block_len, block_len), dtype=bool))[None, :, :, None]

    def advance(carried, inputs):
        state_stack, running = carried
        block_queries, key_block, block_values, decay_block = inputs
        prefix_decay = jnp.cumsum(decay_block, axis=1)
        state_contribution = jnp.einsum('yga,yau->ygu', block_queries * jnp.exp(prefix_decay), state_stack, precision=EXACT_PRECISION)
        relative = prefix_decay[:, :, None, :] - prefix_decay[:, None, :, :]
        decays = jnp.exp(jnp.where(causal_mask, relative, -jnp.inf))
        scores = jnp.einsum('htk,hsk,htsk->hts', block_queries, key_block, decays, precision=EXACT_PRECISION)
        inside = jnp.einsum('hts,hsv->htv', scores, block_values, precision=EXACT_PRECISION)
        total_blocks = prefix_decay[:, -1, :]
        weighted_scores = key_block * jnp.exp(total_blocks[:, None, :] - prefix_decay)
        state_stack = jnp.exp(total_blocks)[:, :, None] * state_stack + jnp.einsum('xpf,xpq->xfq', weighted_scores, block_values, precision=EXACT_PRECISION)
        reached_state = block_queries * jnp.exp(running[:, None, :] + prefix_decay)
        return ((state_stack, running + total_blocks), (state_contribution + inside, reached_state))
    initial = (jnp.zeros((count_heads, key_width, value_width), jnp.float32), jnp.zeros((count_heads, key_width), jnp.float32))
    last_carry, (output_rows, reached_state) = lax.scan(advance, initial, (to_blocks(probe_entries), to_blocks(address_entries), to_blocks(content_arrays), to_blocks(log_fade_amount)))

    def from_blocks(tensor):
        return jnp.moveaxis(tensor, 1, 2).reshape(length, count_heads, tensor.shape[3])
    return (from_blocks(output_rows), from_blocks(reached_state), last_carry)

def head_norm(output_rows, channel_norm_scale, gate_rows):
    inverse = lax.rsqrt(lax.optimization_barrier(jnp.mean(output_rows * output_rows, axis=2, keepdims=True)) + EPSILON)
    normed = (output_rows * inverse * channel_norm_scale).reshape(output_rows.shape[0], -1)
    return (normed * jax.nn.silu(gate_rows.astype(jnp.float32))).astype(jnp.bfloat16)

def reference(layer_source, broad_probe_tensor, broad_retention_preact, broad_floor_margin, slim_probe_tensor, slim_retention_preact, slim_floor_margin, branch_content_tensor, emitted_switch_preact, extra_log_fades, channel_norm_scale, emission_projection, mlp_norm_scale, switch_projection, expand_projection, shrink_projection):
    groups = ((broad_probe_tensor, broad_retention_preact, broad_floor_margin), (slim_probe_tensor, slim_retention_preact, slim_floor_margin))
    branch = jnp.zeros(layer_source.shape, jnp.float32)
    for element_ordinal in range(2):
        probe_array, retention_sigmoid, floor_margin = groups[element_ordinal]
        probe_entries, address_entries, log_fade_amount, content_arrays = switched_token_entries(probe_array, retention_sigmoid, floor_margin, extra_log_fades[element_ordinal], branch_content_tensor[element_ordinal], BRANCH_CHANNELS)
        output_rows, reached_state, last_carry = block_recurrence(probe_entries, address_entries, log_fade_amount, content_arrays, BLOCK)
        mixed = head_norm(output_rows, channel_norm_scale, emitted_switch_preact[element_ordinal])
        branch = branch + jnp.dot(mixed, emission_projection[element_ordinal], preferred_element_type=jnp.float32)
    updated = layer_source.astype(jnp.float32) + branch
    inverse = lax.rsqrt(lax.optimization_barrier(jnp.mean(updated * updated, axis=1, keepdims=True)) + EPSILON)
    normed = (updated * inverse * mlp_norm_scale).astype(jnp.bfloat16)
    gate_part = jnp.dot(normed, switch_projection, preferred_element_type=jnp.float32)
    up_part = jnp.dot(normed, expand_projection, preferred_element_type=jnp.float32)
    hidden = (jax.nn.silu(gate_part) * up_part).astype(jnp.bfloat16)
    ffn_sum = jnp.dot(hidden, shrink_projection, preferred_element_type=jnp.float32)
    return (updated + 0.5 * ffn_sum).astype(jnp.bfloat16)
```

```python
import functools

import jax
import jax.numpy as jnp
from jax import lax
from jax.experimental import pallas as pl
from jax.experimental.pallas import tpu as pltpu
from jax.sharding import PartitionSpec as P


CHUNK = 128
EPSILON = 1e-06
EXACT = lax.Precision.HIGHEST
F32 = jnp.float32
BF16 = jnp.bfloat16


def nt(a, b):
    return lax.dot_general(a, b, (((1,), (1,)), ((), ())), preferred_element_type=F32)


def tn(a, b):
    return lax.dot_general(a, b, (((0,), (0,)), ((), ())), preferred_element_type=F32)


def front_kernel(
    sp,
    tp,
    q0, f0, gap0, q1, f1, gap1, content, switch, fades, head_scale, source, emission, mlp_scale,
    updated_ref, rows_ref,
    logs0, logs1, fade_cum, state0, state1, run0, run1, intra, out_bound, inbox, mixed, regrouped, full,
    state_send, state_recv, mix_send, mix_recv, far_send, far_recv, near_send, near_recv, put_sem,
):
    sp_me, tp_me = lax.axis_index("sp"), lax.axis_index("tp")
    length = q0.shape[0]
    chunks = length // CHUNK
    block = length // tp
    values = content.shape[2]
    half = values // 2
    groups = ((q0, f0, gap0, logs0, state0, run0), (q1, f1, gap1, logs1, state1, run1))

    barrier = pltpu.get_barrier_semaphore()

    def greet_sp(d, carry):
        pl.semaphore_signal(barrier, inc=1, device_id={"sp": lax.rem(sp_me + d, sp)})
        return carry

    def greet_tp(d, carry):
        pl.semaphore_signal(barrier, inc=1, device_id={"tp": lax.rem(tp_me + d, tp)})
        return carry

    lax.fori_loop(1, sp, greet_sp, 0)
    lax.fori_loop(1, tp, greet_tp, 0)
    pl.semaphore_wait(barrier, sp - 1 + tp - 1)

    row_id = lax.broadcasted_iota(jnp.int32, (CHUNK, CHUNK), 0)
    col_id = lax.broadcasted_iota(jnp.int32, (CHUNK, CHUNK), 1)
    causal = row_id >= col_id
    lower = causal.astype(F32)
    upper = (row_id <= col_id).astype(F32)
    for g in range(2):
        fade_cum[g] = jnp.dot(fades[g], upper, precision=EXACT, preferred_element_type=F32)

    def fade_square(g, c):
        across = jnp.broadcast_to(fade_cum[g, pl.ds(c, 1), :], (CHUNK, CHUNK))
        return across, across.T

    def keys_of(f, gap, rows):
        return gap[...] * jax.nn.sigmoid(-f[rows, :].astype(F32))

    totals = []
    for g, (q, f, gap, logs, state, run) in enumerate(groups):
        width = q.shape[1]
        held = jnp.zeros((values, width), F32)
        passed = jnp.zeros((1, width), F32)
        for c in range(chunks):
            rows = pl.ds(c * CHUNK, CHUNK)
            keys = keys_of(f, gap, rows)
            cum = jnp.dot(lower, jnp.log1p(-keys), precision=EXACT, preferred_element_type=F32)
            logs[rows, :] = cum
            down = fade_square(g, c)[1][:, :width]
            total = cum[CHUNK - 1 :, :] + down[CHUNK - 1 :, :]
            state[c] = held
            run[pl.ds(c, 1), :] = passed
            weighted = (keys * jnp.exp(total - cum - down)).astype(BF16)
            held = jnp.exp(total) * held + tn(content[g, rows, :], weighted)
            passed = passed + total
        totals.append((held, passed))

    (wide, wide_log), (narrow, narrow_log) = totals
    out_bound[0:values, :] = wide.astype(BF16)
    out_bound[values : values + half, :] = jnp.concatenate([narrow[:half], narrow[half:]], axis=1).astype(BF16)
    padded = jnp.concatenate([narrow_log, jnp.zeros_like(narrow_log)], axis=1)
    stack = jnp.concatenate([wide_log, padded], axis=0)
    high = stack.astype(BF16).astype(F32)
    mid = (stack - high).astype(BF16).astype(F32)
    low = stack - high - mid
    out_bound[values + half :, :] = jnp.concatenate(
        [high, mid, low, jnp.zeros((10, values), F32)], axis=0
    ).astype(BF16)

    def state_copy(d, target):
        return pltpu.make_async_remote_copy(
            src_ref=out_bound,
            dst_ref=inbox.at[d - 1],
            send_sem=state_send.at[d - 1],
            recv_sem=state_recv.at[d - 1],
            device_id={"sp": target},
        )

    def send_state(d, carry):
        state_copy(d, sp_me + d).start()
        return carry

    lax.fori_loop(1, sp - sp_me, send_state, 0)

    for g, (q, f, gap, logs, state, run) in enumerate(groups):
        width = q.shape[1]
        for c in range(chunks):
            rows = pl.ds(c * CHUNK, CHUNK)
            cum = logs[rows, :]
            across, down = fade_square(g, c)
            query = jax.nn.silu(q[rows, :].astype(F32)) * (width**-0.5) * jnp.exp(cum)
            keys = keys_of(f, gap, rows) * jnp.exp(-cum)
            scores = nt(query.astype(BF16), keys.astype(BF16))
            decay = jnp.exp(jnp.where(causal, down - across, -jnp.inf))
            inside = jnp.dot((scores * decay).astype(BF16), content[g, rows, :], preferred_element_type=F32)
            intra[g, rows, :] = inside
            logs[rows, :] = query * jnp.exp(down[:, :width])

    def gather_state(d, carry):
        held0, between0, held1, between1 = carry
        state_copy(d, sp_me).wait_recv()
        slot = inbox[d - 1].astype(F32)
        got1 = jnp.concatenate(
            [slot[values : values + half, :half], slot[values : values + half, half:]], axis=0
        )
        base = values + half
        log0 = slot[base : base + 1] + slot[base + 2 : base + 3] + slot[base + 4 : base + 5]
        log1 = slot[base + 1 : base + 2] + slot[base + 3 : base + 4] + slot[base + 5 : base + 6]
        held0 = held0 + jnp.exp(between0) * slot[:values]
        held1 = held1 + jnp.exp(between1) * got1
        return held0, between0 + log0, held1, between1 + log1[:, :half]

    zero = (
        jnp.zeros((values, q0.shape[1]), F32),
        jnp.zeros((1, q0.shape[1]), F32),
        jnp.zeros((values, q1.shape[1]), F32),
        jnp.zeros((1, q1.shape[1]), F32),
    )
    entered0, _, entered1, _ = lax.fori_loop(1, sp_me + 1, gather_state, zero)
    entered = (entered0, entered1)

    def mix_copy(step):
        target = lax.rem(tp_me + step, tp)
        return pltpu.make_async_remote_copy(
            src_ref=mixed.at[target],
            dst_ref=regrouped.at[step - 1],
            send_sem=mix_send.at[step - 1],
            recv_sem=mix_recv.at[step - 1],
            device_id={"tp": target},
        )

    for step in list(range(1, tp)) + [0]:
        owner = lax.rem(tp_me + step, tp)

        def one(i, carry):
            c = owner * (block // CHUNK) + i
            rows = pl.ds(pl.multiple_of(c * CHUNK, CHUNK), CHUNK)
            for g, (q, f, gap, logs, state, run) in enumerate(groups):
                full_state = state[c] + jnp.exp(run[pl.ds(c, 1), :]) * entered[g]
                out = intra[g, rows, :] + nt(logs[rows, :].astype(BF16), full_state.astype(BF16))
                scale = lax.rsqrt(jnp.mean(out * out, axis=1, keepdims=True) + EPSILON)
                gated = out * scale * head_scale[...] * jax.nn.silu(switch[g, rows, :].astype(F32))
                mixed[owner, pl.ds(pl.multiple_of(i * CHUNK, CHUNK), CHUNK), pl.ds(g * values, values)] = gated.astype(BF16)
            return carry

        lax.fori_loop(0, block // CHUNK, one, 0)
        if step:
            mix_copy(step).start()

    width = source.shape[1]
    for step in range(tp):
        owner = lax.rem(tp_me - step + tp, tp)
        if step:
            mix_copy(step).wait_recv()
        for g in range(2):
            part = mixed[owner, :, pl.ds(g * values, values)] if step == 0 else regrouped[step - 1, :, pl.ds(g * values, values)]
            weight = emission[g, pl.ds(pl.multiple_of(owner * values, values), values), :]
            product = jnp.dot(part, weight, preferred_element_type=F32)
            if step == 0 and g == 0:
                updated_ref[...] = source[...].astype(F32) + product
            else:
                updated_ref[...] += product
    new = updated_ref[...]
    inverse = lax.rsqrt(jnp.mean(new * new, axis=1, keepdims=True) + EPSILON)
    full[tp_me] = (new * inverse * mlp_scale[...]).astype(BF16)

    near = tp_me + 1 - 2 * lax.rem(tp_me, 2)
    far_count = tp // 2 - 1

    def far_copy(k):
        return pltpu.make_async_remote_copy(
            src_ref=full.at[tp_me],
            dst_ref=full.at[tp_me],
            send_sem=far_send.at[k - 1],
            recv_sem=far_recv.at[k - 1],
            device_id={"tp": lax.rem(tp_me + 2 * k, tp)},
        )

    def near_copy(k, slot):
        return pltpu.make_async_remote_copy(
            src_ref=full.at[slot],
            dst_ref=full.at[slot],
            send_sem=near_send.at[k],
            recv_sem=near_recv.at[k],
            device_id={"tp": near},
        )

    for k in range(1, far_count + 1):
        far_copy(k).start()
    near_copy(0, tp_me).start()
    for k in range(1, far_count + 1):
        slot = lax.rem(tp_me - 2 * k + tp, tp)
        far_copy(k).wait_recv()
        near_copy(k, slot).start()

    def put(k, slot):
        return pltpu.make_async_copy(full.at[slot], rows_ref.at[slot], put_sem.at[k])

    put(0, tp_me).start()
    for k in range(1, far_count + 1):
        put(k, lax.rem(tp_me - 2 * k + tp, tp)).start()
    for k in range(far_count + 1):
        near_copy(k, tp_me).wait_recv()
        put(far_count + 1 + k, lax.rem(near - 2 * k + tp, tp)).start()
    for k in range(tp):
        put(k, tp_me).wait()

    def drain(d, carry):
        state_copy(d, sp_me).wait_send()
        return carry

    lax.fori_loop(1, sp - sp_me, drain, 0)
    for step in range(1, tp):
        mix_copy(step).wait_send()
    for k in range(1, far_count + 1):
        far_copy(k).wait_send()
    for k in range(far_count + 1):
        near_copy(k, tp_me).wait_send()


def front(sp, tp, source, q0, f0, gap0, q1, f1, gap1, content, switch, fades, head_scale, emission, mlp_scale):
    length = q0.shape[0]
    rows, width = source.shape
    values = content.shape[2]
    block = length // tp
    chunks = length // CHUNK
    packed = values + values // 2 + 16
    far = max(tp // 2 - 1, 1)
    vmem = pl.BlockSpec(memory_space=pltpu.VMEM)
    dma = pltpu.SemaphoreType.DMA
    return pl.pallas_call(
        functools.partial(front_kernel, sp, tp),
        out_shape=(
            jax.ShapeDtypeStruct((rows, width), F32),
            jax.ShapeDtypeStruct((tp, block, width), BF16),
        ),
        in_specs=[vmem] * 13,
        out_specs=(vmem, pl.BlockSpec(memory_space=pl.ANY)),
        scratch_shapes=[
            pltpu.VMEM(q0.shape, F32),
            pltpu.VMEM(q1.shape, F32),
            pltpu.VMEM((2, chunks, CHUNK), F32),
            pltpu.VMEM((chunks, values, q0.shape[1]), F32),
            pltpu.VMEM((chunks, values, q1.shape[1]), F32),
            pltpu.VMEM((chunks, q0.shape[1]), F32),
            pltpu.VMEM((chunks, q1.shape[1]), F32),
            pltpu.VMEM((2, length, values), F32),
            pltpu.VMEM((packed, values), BF16),
            pltpu.VMEM((sp - 1, packed, values), BF16),
            pltpu.VMEM((tp, block, 2 * values), BF16),
            pltpu.VMEM((tp - 1, block, 2 * values), BF16),
            pltpu.VMEM((tp, block, width), BF16),
            dma((sp - 1,)), dma((sp - 1,)),
            dma((tp - 1,)), dma((tp - 1,)),
            dma((far,)), dma((far,)),
            dma((far + 1,)), dma((far + 1,)),
            dma((tp,)),
        ],
        compiler_params=pltpu.CompilerParams(
            collective_id=0, has_side_effects=True, vmem_limit_bytes=48 * 1024 * 1024
        ),
        cost_estimate=pl.CostEstimate(flops=400_000_000_000, bytes_accessed=20_000_000, transcendentals=0),
        name="front",
    )(
        q0, f0, gap0.reshape(1, -1), q1, f1, gap1.reshape(1, -1), content, switch,
        fades.reshape(2, chunks, CHUNK), head_scale.reshape(1, -1), source, emission, mlp_scale.reshape(1, -1),
    )


def local(
    layer_source,
    broad_probe_tensor,
    broad_retention_preact,
    broad_floor_margin,
    slim_probe_tensor,
    slim_retention_preact,
    slim_floor_margin,
    branch_content_tensor,
    emitted_switch_preact,
    extra_log_fades,
    channel_norm_scale,
    emission_projection,
    mlp_norm_scale,
    switch_projection,
    expand_projection,
    shrink_projection,
):
    sp, tp = lax.axis_size("sp"), lax.axis_size("tp")
    gate_full = lax.all_gather(switch_projection, "sp", axis=0, tiled=True)
    up_full = lax.all_gather(expand_projection, "sp", axis=0, tiled=True)
    down_full = lax.all_gather(shrink_projection, "sp", axis=1, tiled=True)
    updated, rows = front(
        sp, tp, layer_source, broad_probe_tensor, broad_retention_preact, broad_floor_margin,
        slim_probe_tensor, slim_retention_preact, slim_floor_margin, branch_content_tensor,
        emitted_switch_preact, extra_log_fades, channel_norm_scale, emission_projection, mlp_norm_scale,
    )
    rows = rows.reshape(-1, rows.shape[2])
    gate_part = jnp.dot(rows, gate_full, preferred_element_type=F32)
    up_part = jnp.dot(rows, up_full, preferred_element_type=F32)
    hidden = (jax.nn.silu(gate_part) * up_part).astype(BF16)
    partial = jnp.dot(hidden, down_full, preferred_element_type=F32).astype(BF16)
    ffn_sum = lax.psum_scatter(partial, "tp", scatter_dimension=0, tiled=True).astype(F32)
    return (updated + 0.5 * ffn_sum).astype(BF16)


def solution(mesh):
    placed = (
        P(("sp", "tp"), None),
        P("sp", "tp"),
        P("sp", "tp"),
        P("tp"),
        P("sp", "tp"),
        P("sp", "tp"),
        P("tp"),
        P(None, "sp", "tp"),
        P(None, "sp", "tp"),
        P(None, "sp", "tp"),
        P(),
        P(),
        P(),
        P("sp", "tp"),
        P("sp", "tp"),
        P("tp", "sp"),
    )
    return jax.shard_map(
        local, mesh=mesh, in_specs=placed, out_specs=P(("sp", "tp"), None), check_vma=False
    )
```

```python
import functools

import jax
import jax.numpy as jnp
from jax import lax
from jax.experimental import pallas as pl
from jax.experimental.pallas import tpu as pltpu
from jax.sharding import PartitionSpec as P


CHUNK = 128
EPSILON = 1e-06
EXACT = lax.Precision.HIGHEST
F32 = jnp.float32
BF16 = jnp.bfloat16


def nt(a, b):
    return lax.dot_general(a, b, (((1,), (1,)), ((), ())), preferred_element_type=F32)


def tn(a, b):
    return lax.dot_general(a, b, (((0,), (0,)), ((), ())), preferred_element_type=F32)


def front_kernel(
    sp,
    tp,
    q0, f0, gap0, q1, f1, gap1, content, switch, fades, head_scale, source, emission, mlp_scale,
    updated_ref, rows_ref,
    logs0, logs1, fade_cum, state0, state1, run0, run1, intra, out_bound, inbox, mixed, regrouped, full,
    state_send, state_recv, mix_send, mix_recv, far_send, far_recv, near_send, near_recv, put_sem,
):
    sp_me, tp_me = lax.axis_index("sp"), lax.axis_index("tp")
    length = q0.shape[0]
    chunks = length // CHUNK
    block = length // tp
    values = content.shape[2]
    half = values // 2
    groups = ((q0, f0, gap0, logs0, state0, run0), (q1, f1, gap1, logs1, state1, run1))

    barrier = pltpu.get_barrier_semaphore()

    def greet_sp(d, carry):
        pl.semaphore_signal(barrier, inc=1, device_id={"sp": lax.rem(sp_me + d, sp)})
        return carry

    def greet_tp(d, carry):
        pl.semaphore_signal(barrier, inc=1, device_id={"tp": lax.rem(tp_me + d, tp)})
        return carry

    lax.fori_loop(1, sp, greet_sp, 0)
    lax.fori_loop(1, tp, greet_tp, 0)
    pl.semaphore_wait(barrier, sp - 1 + tp - 1)

    row_id = lax.broadcasted_iota(jnp.int32, (CHUNK, CHUNK), 0)
    col_id = lax.broadcasted_iota(jnp.int32, (CHUNK, CHUNK), 1)
    causal = row_id >= col_id
    lower = causal.astype(F32)
    upper = (row_id <= col_id).astype(F32)
    for g in range(2):
        fade_cum[g] = jnp.dot(fades[g], upper, precision=EXACT, preferred_element_type=F32)

    def fade_square(g, c):
        across = jnp.broadcast_to(fade_cum[g, pl.ds(c, 1), :], (CHUNK, CHUNK))
        return across, across.T

    def keys_of(f, gap, rows):
        return gap[...] * jax.nn.sigmoid(-f[rows, :].astype(F32))

    totals = []
    for g, (q, f, gap, logs, state, run) in enumerate(groups):
        width = q.shape[1]
        held = jnp.zeros((values, width), F32)
        passed = jnp.zeros((1, width), F32)
        for c in range(chunks):
            rows = pl.ds(c * CHUNK, CHUNK)
            keys = keys_of(f, gap, rows)
            cum = jnp.dot(lower, jnp.log1p(-keys), precision=EXACT, preferred_element_type=F32)
            logs[rows, :] = cum
            down = fade_square(g, c)[1][:, :width]
            total = cum[CHUNK - 1 :, :] + down[CHUNK - 1 :, :]
            state[c] = held
            run[pl.ds(c, 1), :] = passed
            weighted = (keys * jnp.exp(total - cum - down)).astype(BF16)
            held = jnp.exp(total) * held + tn(content[g, rows, :], weighted)
            passed = passed + total
        totals.append((held, passed))

    (wide, wide_log), (narrow, narrow_log) = totals
    out_bound[0:values, :] = wide.astype(BF16)
    out_bound[values : values + half, :] = jnp.concatenate([narrow[:half], narrow[half:]], axis=1).astype(BF16)
    padded = jnp.concatenate([narrow_log, jnp.zeros_like(narrow_log)], axis=1)
    stack = jnp.concatenate([wide_log, padded], axis=0)
    high = stack.astype(BF16).astype(F32)
    mid = (stack - high).astype(BF16).astype(F32)
    low = stack - high - mid
    out_bound[values + half :, :] = jnp.concatenate(
        [high, mid, low, jnp.zeros((10, values), F32)], axis=0
    ).astype(BF16)

    def state_copy(d, target):
        return pltpu.make_async_remote_copy(
            src_ref=out_bound,
            dst_ref=inbox.at[d - 1],
            send_sem=state_send.at[d - 1],
            recv_sem=state_recv.at[d - 1],
            device_id={"sp": target},
        )

    def send_state(d, carry):
        state_copy(d, sp_me + d).start()
        return carry

    lax.fori_loop(1, sp - sp_me, send_state, 0)

    for g, (q, f, gap, logs, state, run) in enumerate(groups):
        width = q.shape[1]
        for c in range(chunks):
            rows = pl.ds(c * CHUNK, CHUNK)
            cum = logs[rows, :]
            across, down = fade_square(g, c)
            query = jax.nn.silu(q[rows, :].astype(F32)) * (width**-0.5) * jnp.exp(cum)
            keys = keys_of(f, gap, rows) * jnp.exp(-cum)
            scores = nt(query.astype(BF16), keys.astype(BF16))
            decay = jnp.exp(jnp.where(causal, down - across, -jnp.inf))
            inside = jnp.dot((scores * decay).astype(BF16), content[g, rows, :], preferred_element_type=F32)
            intra[g, rows, :] = inside
            logs[rows, :] = query * jnp.exp(down[:, :width])

    def gather_state(d, carry):
        held0, between0, held1, between1 = carry
        state_copy(d, sp_me).wait_recv()
        slot = inbox[d - 1].astype(F32)
        got1 = jnp.concatenate(
            [slot[values : values + half, :half], slot[values : values + half, half:]], axis=0
        )
        base = values + half
        log0 = slot[base : base + 1] + slot[base + 2 : base + 3] + slot[base + 4 : base + 5]
        log1 = slot[base + 1 : base + 2] + slot[base + 3 : base + 4] + slot[base + 5 : base + 6]
        held0 = held0 + jnp.exp(between0) * slot[:values]
        held1 = held1 + jnp.exp(between1) * got1
        return held0, between0 + log0, held1, between1 + log1[:, :half]

    zero = (
        jnp.zeros((values, q0.shape[1]), F32),
        jnp.zeros((1, q0.shape[1]), F32),
        jnp.zeros((values, q1.shape[1]), F32),
        jnp.zeros((1, q1.shape[1]), F32),
    )
    entered0, _, entered1, _ = lax.fori_loop(1, sp_me + 1, gather_state, zero)
    entered = (entered0, entered1)

    def mix_copy(step):
        target = lax.rem(tp_me + step, tp)
        return pltpu.make_async_remote_copy(
            src_ref=mixed.at[target],
            dst_ref=regrouped.at[step - 1],
            send_sem=mix_send.at[step - 1],
            recv_sem=mix_recv.at[step - 1],
            device_id={"tp": target},
        )

    for step in list(range(1, tp)) + [0]:
        owner = lax.rem(tp_me + step, tp)

        def one(i, carry):
            c = owner * (block // CHUNK) + i
            rows = pl.ds(pl.multiple_of(c * CHUNK, CHUNK), CHUNK)
            for g, (q, f, gap, logs, state, run) in enumerate(groups):
                full_state = state[c] + jnp.exp(run[pl.ds(c, 1), :]) * entered[g]
                out = intra[g, rows, :] + nt(logs[rows, :].astype(BF16), full_state.astype(BF16))
                scale = lax.rsqrt(jnp.mean(out * out, axis=1, keepdims=True) + EPSILON)
                gated = out * scale * head_scale[...] * jax.nn.silu(switch[g, rows, :].astype(F32))
                mixed[owner, pl.ds(pl.multiple_of(i * CHUNK, CHUNK), CHUNK), pl.ds(g * values, values)] = gated.astype(BF16)
            return carry

        lax.fori_loop(0, block // CHUNK, one, 0)
        if step:
            mix_copy(step).start()

    width = source.shape[1]
    for step in range(tp):
        owner = lax.rem(tp_me - step + tp, tp)
        if step:
            mix_copy(step).wait_recv()
        for g in range(2):
            part = mixed[owner, :, pl.ds(g * values, values)] if step == 0 else regrouped[step - 1, :, pl.ds(g * values, values)]
            weight = emission[g, pl.ds(pl.multiple_of(owner * values, values), values), :]
            product = jnp.dot(part, weight, preferred_element_type=F32)
            if step == 0 and g == 0:
                updated_ref[...] = source[...].astype(F32) + product
            else:
                updated_ref[...] += product
    new = updated_ref[...]
    inverse = lax.rsqrt(jnp.mean(new * new, axis=1, keepdims=True) + EPSILON)
    full[tp_me] = (new * inverse * mlp_scale[...]).astype(BF16)

    near = tp_me + 1 - 2 * lax.rem(tp_me, 2)
    far_count = tp // 2 - 1

    def far_copy(k):
        return pltpu.make_async_remote_copy(
            src_ref=full.at[tp_me],
            dst_ref=full.at[tp_me],
            send_sem=far_send.at[k - 1],
            recv_sem=far_recv.at[k - 1],
            device_id={"tp": lax.rem(tp_me + 2 * k, tp)},
        )

    def near_copy(k, slot):
        return pltpu.make_async_remote_copy(
            src_ref=full.at[slot],
            dst_ref=full.at[slot],
            send_sem=near_send.at[k],
            recv_sem=near_recv.at[k],
            device_id={"tp": near},
        )

    for k in range(1, far_count + 1):
        far_copy(k).start()
    near_copy(0, tp_me).start()
    for k in range(1, far_count + 1):
        slot = lax.rem(tp_me - 2 * k + tp, tp)
        far_copy(k).wait_recv()
        near_copy(k, slot).start()

    def put(k, slot):
        return pltpu.make_async_copy(full.at[slot], rows_ref.at[slot], put_sem.at[k])

    put(0, tp_me).start()
    for k in range(1, far_count + 1):
        put(k, lax.rem(tp_me - 2 * k + tp, tp)).start()
    for k in range(far_count + 1):
        near_copy(k, tp_me).wait_recv()
        put(far_count + 1 + k, lax.rem(near - 2 * k + tp, tp)).start()
    for k in range(tp):
        put(k, tp_me).wait()

    def drain(d, carry):
        state_copy(d, sp_me).wait_send()
        return carry

    lax.fori_loop(1, sp - sp_me, drain, 0)
    for step in range(1, tp):
        mix_copy(step).wait_send()
    for k in range(1, far_count + 1):
        far_copy(k).wait_send()
    for k in range(far_count + 1):
        near_copy(k, tp_me).wait_send()


def front(sp, tp, source, q0, f0, gap0, q1, f1, gap1, content, switch, fades, head_scale, emission, mlp_scale):
    length = q0.shape[0]
    rows, width = source.shape
    values = content.shape[2]
    block = length // tp
    chunks = length // CHUNK
    packed = values + values // 2 + 16
    far = max(tp // 2 - 1, 1)
    vmem = pl.BlockSpec(memory_space=pltpu.VMEM)
    dma = pltpu.SemaphoreType.DMA
    return pl.pallas_call(
        functools.partial(front_kernel, sp, tp),
        out_shape=(
            jax.ShapeDtypeStruct((rows, width), F32),
            jax.ShapeDtypeStruct((tp, block, width), BF16),
        ),
        in_specs=[vmem] * 13,
        out_specs=(vmem, pl.BlockSpec(memory_space=pl.ANY)),
        scratch_shapes=[
            pltpu.VMEM(q0.shape, F32),
            pltpu.VMEM(q1.shape, F32),
            pltpu.VMEM((2, chunks, CHUNK), F32),
            pltpu.VMEM((chunks, values, q0.shape[1]), F32),
            pltpu.VMEM((chunks, values, q1.shape[1]), F32),
            pltpu.VMEM((chunks, q0.shape[1]), F32),
            pltpu.VMEM((chunks, q1.shape[1]), F32),
            pltpu.VMEM((2, length, values), F32),
            pltpu.VMEM((packed, values), BF16),
            pltpu.VMEM((sp - 1, packed, values), BF16),
            pltpu.VMEM((tp, block, 2 * values), BF16),
            pltpu.VMEM((tp - 1, block, 2 * values), BF16),
            pltpu.VMEM((tp, block, width), BF16),
            dma((sp - 1,)), dma((sp - 1,)),
            dma((tp - 1,)), dma((tp - 1,)),
            dma((far,)), dma((far,)),
            dma((far + 1,)), dma((far + 1,)),
            dma((tp,)),
        ],
        compiler_params=pltpu.CompilerParams(
            collective_id=0, has_side_effects=True, vmem_limit_bytes=48 * 1024 * 1024
        ),
        cost_estimate=pl.CostEstimate(flops=400_000_000_000, bytes_accessed=20_000_000, transcendentals=0),
        name="front",
    )(
        q0, f0, gap0.reshape(1, -1), q1, f1, gap1.reshape(1, -1), content, switch,
        fades.reshape(2, chunks, CHUNK), head_scale.reshape(1, -1), source, emission, mlp_scale.reshape(1, -1),
    )


def local(
    layer_source,
    broad_probe_tensor,
    broad_retention_preact,
    broad_floor_margin,
    slim_probe_tensor,
    slim_retention_preact,
    slim_floor_margin,
    branch_content_tensor,
    emitted_switch_preact,
    extra_log_fades,
    channel_norm_scale,
    emission_projection,
    mlp_norm_scale,
    switch_projection,
    expand_projection,
    shrink_projection,
):
    sp, tp = lax.axis_size("sp"), lax.axis_size("tp")
    groups = [[i for i in range(sp) if i % 2 == r] for r in range(2)]
    swap = [(i, i ^ 1) for i in range(sp)]
    gate_own = lax.all_gather(switch_projection, "sp", axis=0, tiled=True, axis_index_groups=groups)
    up_own = lax.all_gather(expand_projection, "sp", axis=0, tiled=True, axis_index_groups=groups)
    down_full = lax.all_gather(shrink_projection, "sp", axis=1, tiled=True)
    updated, rows = front(
        sp, tp, layer_source, broad_probe_tensor, broad_retention_preact, broad_floor_margin,
        slim_probe_tensor, slim_retention_preact, slim_floor_margin, branch_content_tensor,
        emitted_switch_preact, extra_log_fades, channel_norm_scale, emission_projection, mlp_norm_scale,
    )
    gate_other = lax.ppermute(gate_own, "sp", swap)
    up_other = lax.ppermute(up_own, "sp", swap)
    piece = switch_projection.shape[0]
    parity = lax.rem(lax.axis_index("sp"), 2)
    pieces = rows.reshape(-1, sp // 2, 2, piece)

    def columns(which):
        picked = lax.dynamic_index_in_dim(pieces, which, 2, False)
        return picked.reshape(picked.shape[0], -1)

    own, other = lax.optimization_barrier((columns(parity), columns(1 - parity)))
    gate_part = jnp.dot(own, gate_own, preferred_element_type=F32)
    gate_part = gate_part + jnp.dot(other, gate_other, preferred_element_type=F32)
    up_part = jnp.dot(own, up_own, preferred_element_type=F32)
    up_part = up_part + jnp.dot(other, up_other, preferred_element_type=F32)
    hidden = (jax.nn.silu(gate_part) * up_part).astype(BF16)
    hidden = lax.optimization_barrier(hidden)
    partial = jnp.dot(hidden, down_full, preferred_element_type=F32).astype(BF16)
    ffn_sum = lax.psum_scatter(partial, "tp", scatter_dimension=0, tiled=True).astype(F32)
    return (updated + 0.5 * ffn_sum).astype(BF16)


def solution(mesh):
    placed = (
        P(("sp", "tp"), None),
        P("sp", "tp"),
        P("sp", "tp"),
        P("tp"),
        P("sp", "tp"),
        P("sp", "tp"),
        P("tp"),
        P(None, "sp", "tp"),
        P(None, "sp", "tp"),
        P(None, "sp", "tp"),
        P(),
        P(),
        P(),
        P("sp", "tp"),
        P("sp", "tp"),
        P("tp", "sp"),
    )
    return jax.shard_map(
        local, mesh=mesh, in_specs=placed, out_specs=P(("sp", "tp"), None), check_vma=False
    )
```
